32 devices in a mesh: sp: 16 (over z, y, x), tp: 2 (over core).
Axes of the slice: x: 2, y: 2, z: 4, core: 2. Of those that a mesh axis runs over, the one named last changes fastest.
Arguments:
- tokens: bfloat16 [16384, 2048], P('sp', 'tp'), may hold values from -6 to 6
- norm_gain: float32 [2048], replicated, may hold values from 0.1 to 1.9
- w_conv_a: bfloat16 [2048, 1024], P('sp', 'tp'), may hold values from -0.125 to 0.125
- w_conv_gate: bfloat16 [2048, 1024], P('sp', 'tp'), may hold values from -0.125 to 0.125
- conv_weight: float32 [31, 1024], P(None, 'tp'), may hold values from -16 to 16
- conv_gain: float32 [1024], P('tp'), may hold values from 0.1 to 1.9
- w_query: bfloat16 [2048, 512], P('sp', 'tp'), may hold values from -0.125 to 0.125
- w_key: bfloat16 [2048, 512], P('sp', 'tp'), may hold values from -0.125 to 0.125
- w_value: bfloat16 [2048, 1024], P('sp', 'tp'), may hold values from -0.125 to 0.125
- w_outgate: bfloat16 [2048, 1024], P('sp', 'tp'), may hold values from -0.125 to 0.125
- w_decay: bfloat16 [2048, 512], P('sp', 'tp'), may hold values from -0.125 to 0.125
- decay_bias: float32 [512], P('tp'), may hold values from 0 to 12
- decay_extra: float32 [16384, 512], P('sp', 'tp'), may hold values from -2 to 0
- head_gain: float32 [128], replicated, may hold values from 0.1 to 1.9
- init_state: float32 [8, 64, 128], P('tp'), may hold values from -768 to 768
- w_out_conv: bfloat16 [1024, 2048], P('tp', 'sp'), may hold values from -0.125 to 0.125
- w_out_gla: bfloat16 [1024, 2048], P('tp', 'sp'), may hold values from -0.125 to 0.125
Outputs:
- mixed: bfloat16 [16384, 2048], P(('sp', 'tp'))
The draws below stay inside these ranges and needn't reach their ends.
All inputs are finite; a program needn't handle non-finite values.
Results may differ from the reference program's by a relative error of at most 0.022.
Values may be sent and summed in bfloat16 or wider, within the bound.
No kernel may reach another device: no remote copies, remote signals or barrier semaphores. Data moves between devices by JAX's collectives and lax.ppermute only.
A program may use at most 128 MiB of HBM per device.

```python
import jax
import jax.numpy as jnp
from jax import lax

D = 2048
D_CONV = 1024
HEADS = 8
HK = 64
HV = 128
KERNEL = 31
BLOCK = 64
TOK_DEV = 1024
SEQUENCE_TOKENS = 16384
GLA_K = 512
GLA_V = 1024
N_TP = 2


def draw_conv_weight(key, part):
    key_base = jax.random.fold_in(key, 0)
    base = jax.random.normal(key_base, (KERNEL, D_CONV), jnp.float32) * KERNEL ** (-0.5)
    rising = 3.0 ** (jnp.arange(D_CONV, dtype=jnp.float32) / (D_CONV - 1))
    return base * rising[None, :]


def draw_decay_bias(key, part):
    key_pick, key_fast, key_slow = jax.random.split(key, 3)
    fast_share = 0.5
    fast_head = jax.random.bernoulli(key_pick, fast_share, (HEADS,))
    fast_values = jax.random.uniform(key_fast, (HEADS, HK), jnp.float32, 0.0, 1.0)
    slow_values = jax.random.uniform(key_slow, (HEADS, HK), jnp.float32, 8.0, 12.0)
    return jnp.where(fast_head[:, None], fast_values, slow_values).reshape(HEADS * HK)


def draw_decay_extra(key, part):
    key_factor, key_location, key_width, key_channel = jax.random.split(key, 4)
    factor = jax.random.uniform(key_factor, (SEQUENCE_TOKENS // TOK_DEV, 1), jnp.float32, 1.0, 3.0)
    row_each = jnp.repeat(factor, TOK_DEV, axis=0)
    channel_index = jax.random.uniform(key_channel, (1, HEADS * HK), jnp.float32, 0.5, 1.5)
    spike_locations = jax.random.randint(key_location, (3,), 0, SEQUENCE_TOKENS)
    spike_depth = jax.random.uniform(key_width, (3, 1), jnp.float32, 0.22, 0.5)
    spike_events = (jnp.arange(SEQUENCE_TOKENS)[:, None] == spike_locations[None, :]).astype(jnp.float32)
    return -(0.4 / SEQUENCE_TOKENS) * row_each * channel_index - jnp.dot(spike_events, spike_depth)


def block_scale(rng, extent, cuts, least, high):
    def one(dim, shards_of):
        steps = jax.random.uniform(jax.random.fold_in(jax.random.fold_in(rng, 6), dim), (shards_of,), jnp.float32, least / len(cuts), high / len(cuts))
        return jnp.repeat(jnp.exp(steps), extent[dim] // shards_of).reshape((-1,) + (1,) * (len(extent) - dim - 1))

    factor_of = one(*cuts[0])
    for cut in cuts[1:]:
        factor_of = factor_of * one(*cut)
    return factor_of


def bell_draw(key, shape, scale, most, shards=(), kind=jnp.bfloat16):
    entries = jax.random.normal(key, shape, jnp.float32) * scale
    if len(shards) > 0:
        entries = block_scale(key, shape, shards, -0.22, 0.18) * entries
    return jnp.clip(entries, min=-most, max=most).astype(kind)


def setup_inputs(seed: int = 0) -> dict:
    streams_of = jax.random.split(jax.random.key(seed), 18)
    return {
        "tokens": bell_draw(streams_of[0], (SEQUENCE_TOKENS, D), 1.0, 6.0, ((0, 16), (1, 2))),
        "norm_gain": jnp.clip(1.0 + 0.18 * jax.random.normal(streams_of[1], (D,), jnp.float32), 0.1, 1.9),
        "w_conv_a": bell_draw(streams_of[2], (D, D_CONV), D ** -0.5, 0.125, ((0, 16), (1, 2))),
        "w_conv_gate": bell_draw(streams_of[3], (D, D_CONV), D ** -0.5, 0.125, ((0, 16), (1, 2))),
        "conv_weight": draw_conv_weight(jax.random.fold_in(streams_of[17], 71), 0),
        "conv_gain": jnp.clip(1.0 + 0.18 * jax.random.normal(streams_of[5], (D_CONV,), jnp.float32), 0.1, 1.9),
        "w_query": bell_draw(streams_of[6], (D, GLA_K), D ** -0.5, 0.125, ((0, 16), (1, 2))),
        "w_key": bell_draw(streams_of[7], (D, GLA_K), D ** -0.5, 0.125, ((0, 16), (1, 2))),
        "w_value": bell_draw(streams_of[8], (D, GLA_V), D ** -0.5, 0.125, ((0, 16), (1, 2))),
        "w_outgate": bell_draw(streams_of[9], (D, GLA_V), D ** -0.5, 0.125, ((0, 16), (1, 2))),
        "w_decay": bell_draw(streams_of[10], (D, GLA_K), D ** -0.5, 0.125, ((0, 16), (1, 2))),
        "decay_bias": draw_decay_bias(jax.random.fold_in(streams_of[17], 71), 0),
        "decay_extra": draw_decay_extra(jax.random.fold_in(streams_of[17], 71), 0),
        "head_gain": jnp.clip(1.0 + 0.18 * jax.random.normal(streams_of[13], (HV,), jnp.float32), 0.1, 1.9),
        "init_state": bell_draw(streams_of[14], (HEADS, HK, HV), (SEQUENCE_TOKENS ** 0.5), 768.0, ((0, 2),), jnp.float32),
        "w_out_conv": bell_draw(streams_of[15], (D_CONV, D), (D_CONV + GLA_V) ** -0.5, 0.125, ((0, 2), (1, 16))),
        "w_out_gla": bell_draw(streams_of[16], (GLA_V, D), (D_CONV + GLA_V) ** -0.5, 0.125, ((0, 2), (1, 16))),
    }


epsilon = 1e-06
gate_divisor = 16.0
highest_precision = lax.Precision.HIGHEST

def project(hidden, weight):
    return jnp.dot(hidden, weight, preferred_element_type=jnp.float32)

def rounded(values_f32):
    return lax.optimization_barrier(values_f32.astype(jnp.bfloat16)).astype(jnp.float32)

def reference(tokens, norm_gain, w_conv_a, w_conv_gate, conv_weight, conv_gain, w_query, w_key, w_value, w_outgate, w_decay, decay_bias, decay_extra, head_gain, init_state, w_out_conv, w_out_gla):
    widened = tokens.astype(jnp.float32)
    normed = (widened * lax.rsqrt(lax.optimization_barrier(jnp.mean(widened * widened, axis=-1, keepdims=True)) + epsilon) * norm_gain).astype(jnp.bfloat16)
    conv_a = rounded(project(normed, w_conv_a))
    conv_gate = rounded(project(normed, w_conv_gate))
    query = rounded(project(normed, w_query))
    keys = rounded(project(normed, w_key))
    values = rounded(project(normed, w_value))
    out_gate = rounded(project(normed, w_outgate))
    decay_pre = project(normed, w_decay)
    gated = rounded(conv_a * jax.nn.sigmoid(conv_gate))
    padded = jnp.pad(gated, ((KERNEL - 1, 0), (0, 0)))
    conv_sum = jnp.zeros((SEQUENCE_TOKENS, D_CONV), jnp.float32)
    for tap_index in range(KERNEL):
        conv_sum = conv_sum + conv_weight[tap_index][None, :] * padded[tap_index:tap_index + SEQUENCE_TOKENS]
    mean_val = lax.optimization_barrier(jnp.mean(conv_sum, axis=-1, keepdims=True))
    square_mean = lax.optimization_barrier(jnp.mean(conv_sum * conv_sum, axis=-1, keepdims=True))
    conv_norm = (conv_sum - mean_val) * lax.rsqrt(square_mean - mean_val * mean_val + epsilon) * conv_gain
    conv_out = jax.nn.silu(conv_norm).astype(jnp.bfloat16)
    log_decay = jax.nn.log_sigmoid(decay_pre + decay_bias) / gate_divisor + decay_extra
    blocks = SEQUENCE_TOKENS // BLOCK

    def to_heads(array, width):
        return array.astype(jnp.float32).reshape(blocks, BLOCK, HEADS, width).transpose(0, 2, 1, 3)
    query_heads = to_heads(query, HK) * HK ** (-0.5)
    key_heads = to_heads(keys, HK)
    value_heads = to_heads(values, HV)
    cum_log = jnp.cumsum(to_heads(log_decay, HK), axis=2)
    block_total = cum_log[:, :, -1:, :]
    query_decayed = query_heads * jnp.exp(cum_log)
    key_inverse = key_heads * jnp.exp(-cum_log)
    key_to_end = key_heads * jnp.exp(block_total - cum_log)
    causal = jnp.tril(jnp.ones((BLOCK, BLOCK), dtype=bool))
    scores = jnp.where(causal, jnp.einsum('nhik,nhjk->nhij', query_decayed, key_inverse, precision=highest_precision), 0.0)
    within = jnp.einsum('nhij,nhjv->nhiv', scores, value_heads, precision=highest_precision)

    def advance(state_current, block_items):
        query_block, key_block, value_block, decay_block = block_items
        carried_state = jnp.einsum('yau,yub->yab', query_block, state_current, precision=highest_precision)
        state_following = state_current * decay_block[:, 0, :, None] + jnp.einsum('tie,tis->tes', key_block, value_block, precision=highest_precision)
        return (state_following, carried_state)
    final_state, carried_out = lax.scan(advance, init_state.astype(jnp.float32), (query_decayed, key_to_end, value_heads, jnp.exp(block_total)))
    attn = within + carried_out
    normal_attn = attn * lax.rsqrt(lax.optimization_barrier(jnp.mean(attn * attn, axis=-1, keepdims=True)) + epsilon) * head_gain
    normal_attn = normal_attn.transpose(0, 2, 1, 3).reshape(SEQUENCE_TOKENS, HEADS * HV)
    gla_out = (normal_attn * jax.nn.silu(out_gate)).astype(jnp.bfloat16)
    conv_share = D_CONV // N_TP
    value_share = HEADS * HV // N_TP
    totals = jnp.zeros((SEQUENCE_TOKENS, D), jnp.float32)
    for group_index in range(N_TP):
        partial_value = project(conv_out[:, group_index * conv_share:(group_index + 1) * conv_share], w_out_conv[group_index * conv_share:(group_index + 1) * conv_share])
        partial_value = partial_value + project(gla_out[:, group_index * value_share:(group_index + 1) * value_share], w_out_gla[group_index * value_share:(group_index + 1) * value_share])
        totals = totals + rounded(partial_value)
    return totals.astype(jnp.bfloat16)
```

```python
import functools

import jax
import jax.numpy as jnp
from jax import lax
from jax.experimental import pallas as pl
from jax.experimental.pallas import tpu as pltpu
from jax.sharding import PartitionSpec as P

HK = 64
HV = 128
BLOCK = 128
LANES = 128
HALO = 32
ROW_TILE = 256
DIRECT = 16


epsilon = 1e-06
gate_divisor = 16.0
f32 = jnp.float32
bf16 = jnp.bfloat16
SMEM = pl.BlockSpec(memory_space=pltpu.SMEM)


def whole(shape):
    return pl.BlockSpec(shape, lambda i: (0,) * len(shape))


def params(megabytes):
    return pltpu.CompilerParams(
        dimension_semantics=("arbitrary",), vmem_limit_bytes=megabytes * 1024 * 1024
    )


def dot(a, b):
    return jnp.dot(a, b, preferred_element_type=f32)


def flip(value, axis, mask):
    count = lax.axis_size(axis)
    return lax.ppermute(value, axis, [(i, i ^ mask) for i in range(count)])


def spread(own, axis, turn):
    count = lax.axis_size(axis)
    masks = [1 << bit for bit in range(count.bit_length() - 1)]
    near, far = masks[:2], masks[2:]
    pieces = {0: own}
    for mask in far:
        for place in list(pieces):
            pieces[place | mask] = flip(pieces[place], axis, mask)
    columns = list(pieces)
    for place in columns:
        for mask in near:
            pieces[place | mask] = flip(pieces[place], axis, mask)
    if len(near) == 2:
        for number, place in enumerate(columns):
            first, last = near if (number + turn) % 2 else near[::-1]
            pieces[place | 3] = flip(pieces[place | last], axis, first)
    return [pieces[place] for place in range(count)]


def gathered(own, axis, dim, turn):
    count = lax.axis_size(axis)
    if count > DIRECT or count & (count - 1):
        return [lax.all_gather(own, axis, axis=dim, tiled=True)], jnp.zeros((1,), jnp.int32)
    order = jnp.arange(count, dtype=jnp.int32)
    return spread(own, axis, turn), (order ^ lax.axis_index(axis)) * own.shape[dim]


def shifted(value, axis, steps):
    count = lax.axis_size(axis)
    return lax.ppermute(value, axis, [(i, i + steps) for i in range(count - steps)])


def chain(earlier, later):
    state = jnp.exp(later[1])[:, None] * earlier[0] + later[0]
    return state, earlier[1] + later[1]


def entering(state, logs, axis):
    count = lax.axis_size(axis)
    rows, channels = state.shape[0], logs.shape[0]
    tail = jnp.zeros((8 * LANES - channels,), f32)

    def pack(pair):
        return jnp.concatenate([pair[0], jnp.concatenate([pair[1], tail]).reshape(8, LANES)])

    def unpack(array):
        return array[:rows], array[rows:].reshape(-1)[:channels]

    before = None
    window = (state, logs)
    stride = 1
    while stride < count:
        packed = pack(window)
        parts = [
            unpack(shifted(packed, axis, stride * k)) for k in (3, 2, 1) if stride * k < count
        ]
        joined = functools.reduce(chain, parts)
        before = joined if before is None else chain(joined, before)
        stride *= 4
        if stride < count:
            window = chain(joined, window)
    return before


def project_body(offs, normed, *refs, pieces, sections):
    weight = refs[-1]
    outs = refs[pieces:-1]

    @pl.when(pl.program_id(0) == 0)
    def _():
        for k in range(pieces):
            rows = refs[k].shape[0]
            weight[pl.ds(pl.multiple_of(offs[k], rows), rows), :] = refs[k][...]

    start = 0
    for out in outs:
        width = out.shape[1]
        out[...] = dot(normed[...], weight[:, start : start + width]).astype(out.dtype)
        start += width


def project(normed, pieces, offs, widths, kinds):
    rows, depth = normed.shape
    total = sum(widths)
    tile = min(ROW_TILE, rows)
    return pl.pallas_call(
        functools.partial(project_body, pieces=len(pieces), sections=len(widths)),
        grid=(rows // tile,),
        in_specs=[SMEM, pl.BlockSpec((tile, depth), lambda i: (i, 0))]
        + [whole(p.shape) for p in pieces],
        out_specs=[pl.BlockSpec((tile, w), lambda i: (i, 0)) for w in widths],
        out_shape=[jax.ShapeDtypeStruct((rows, w), k) for w, k in zip(widths, kinds)],
        scratch_shapes=[pltpu.VMEM((depth, total), bf16)],
        compiler_params=params(36),
        cost_estimate=pl.CostEstimate(
            flops=2 * rows * depth * total, bytes_accessed=rows * depth * 2, transcendentals=0
        ),
        name="project",
    )(offs, normed, *pieces)


def conv_project_body(offs, normed, before, *refs, pieces):
    weight = refs[-1]
    gated, gate_out, rim = refs[pieces:-1]
    width = gated.shape[1]

    def gate(values):
        left = values[:, :width].astype(bf16).astype(f32)
        right = values[:, width : 2 * width].astype(bf16).astype(f32)
        return (left * jax.nn.sigmoid(right)).astype(bf16)

    @pl.when(pl.program_id(0) == 0)
    def _():
        for k in range(pieces):
            rows = refs[k].shape[0]
            weight[pl.ds(pl.multiple_of(offs[k], rows), rows), :] = refs[k][...]
        rim[...] = gate(dot(before[...], weight[:, : 2 * width]))

    gated[...] = gate(dot(normed[...], weight[:, : 2 * width]))
    gate_out[...] = dot(normed[...], weight[:, 2 * width :]).astype(bf16)


def conv_project(normed, before, pieces, offs, width, gate_width):
    rows, depth = normed.shape
    total = 2 * width + gate_width
    tile = min(ROW_TILE, rows)
    return pl.pallas_call(
        functools.partial(conv_project_body, pieces=len(pieces)),
        grid=(rows // tile,),
        in_specs=[SMEM, pl.BlockSpec((tile, depth), lambda i: (i, 0)), whole(before.shape)]
        + [whole(p.shape) for p in pieces],
        out_specs=[
            pl.BlockSpec((tile, width), lambda i: (i, 0)),
            pl.BlockSpec((tile, gate_width), lambda i: (i, 0)),
            whole((before.shape[0], width)),
        ],
        out_shape=[
            jax.ShapeDtypeStruct((rows, width), bf16),
            jax.ShapeDtypeStruct((rows, gate_width), bf16),
            jax.ShapeDtypeStruct((before.shape[0], width), bf16),
        ],
        scratch_shapes=[pltpu.VMEM((depth, total), bf16)],
        compiler_params=params(40),
        cost_estimate=pl.CostEstimate(
            flops=2 * rows * depth * total, bytes_accessed=rows * depth * 2, transcendentals=0
        ),
        name="conv_project",
    )(offs, normed, before, *pieces)


def conv_body(gated, rim, taps, out, sums, extended, moved):
    rows, width = gated.shape
    count = taps.shape[0]
    extended[:HALO] = rim[...].astype(f32)
    extended[HALO : HALO + rows] = gated[...].astype(f32)
    extended[HALO + rows :] = jnp.zeros((8, width), f32)
    first = HALO - count + 1
    chunk = 64
    for residue in range(8):
        moved[residue] = extended[residue : residue + rows + HALO, :]

    def step(i, carry):
        base = pl.multiple_of(i * chunk, chunk)
        total = jnp.zeros((chunk, 1), f32)
        square = jnp.zeros((chunk, 1), f32)
        for lane in range(0, width, LANES):
            acc = jnp.zeros((chunk, LANES), f32)
            for tap in range(count):
                whole_part, residue = divmod(first + tap, 8)
                acc = acc + taps[tap : tap + 1, lane : lane + LANES] * moved[
                    residue, pl.ds(base + 8 * whole_part, chunk), lane : lane + LANES
                ]
            out[pl.ds(base, chunk), lane : lane + LANES] = acc
            total = total + jnp.sum(acc, axis=1, keepdims=True)
            square = square + jnp.sum(acc * acc, axis=1, keepdims=True)
        sums[pl.ds(base, chunk), 0:1] = total
        sums[pl.ds(base, chunk), 1:2] = square
        return carry

    lax.fori_loop(0, rows // chunk, step, 0)


def convolve(gated, rim, taps):
    rows, width = gated.shape
    return pl.pallas_call(
        conv_body,
        out_shape=[
            jax.ShapeDtypeStruct((rows, width), f32),
            jax.ShapeDtypeStruct((rows, 2), f32),
        ],
        scratch_shapes=[
            pltpu.VMEM((HALO + rows + 8, width), f32),
            pltpu.VMEM((8, rows + HALO, width), f32),
        ],
        compiler_params=pltpu.CompilerParams(vmem_limit_bytes=36 * 1024 * 1024),
        cost_estimate=pl.CostEstimate(
            flops=20 * rows * width * taps.shape[0], bytes_accessed=rows * width * 6, transcendentals=0
        ),
        name="convolve",
    )(gated, rim, taps)


def gla_body(query, keys, values, pre, bias, extra, local, since, state_out, logs, state, prefix):
    rows, channels = query.shape
    step = pl.program_id(0)
    group = min(2, channels // HK)
    kw, vw = HK * group, HV * group

    @pl.when(step == 0)
    def _():
        state[...] = jnp.zeros(state.shape, f32)
        prefix[...] = jnp.zeros(prefix.shape, f32)

    biased = pre[...] + bias[...]
    log_decay = (jnp.minimum(biased, 0.0) - jnp.log1p(jnp.exp(-jnp.abs(biased)))) / gate_divisor
    log_decay = log_decay + extra[...]
    at = lax.broadcasted_iota(jnp.int32, (rows, rows), 0)
    by = lax.broadcasted_iota(jnp.int32, (rows, rows), 1)
    causal = at >= by
    cum = jnp.dot(
        causal.astype(f32), log_decay, preferred_element_type=f32, precision=lax.Precision.HIGHEST
    )
    middle = cum[rows // 2 - 1 : rows // 2]
    end = cum[rows - 1 : rows]
    before = prefix[0:1]
    q = query[...].astype(f32) * HK ** (-0.5)
    k = keys[...].astype(f32)
    grown = jnp.exp(cum)
    q_mid = q * jnp.exp(cum - middle)
    k_mid = (k * jnp.exp(middle - cum)).astype(bf16)
    k_end = (k * jnp.exp(end - cum)).astype(bf16)
    q_run = q * grown
    since[...] = (q_run * jnp.exp(before)).astype(bf16)
    q_run = q_run.astype(bf16)
    end_decay = jnp.exp(end)
    key_row = lax.broadcasted_iota(jnp.int32, (kw, kw), 0)
    key_col = lax.broadcasted_iota(jnp.int32, (kw, kw), 1)
    lane = lax.broadcasted_iota(jnp.int32, (rows, kw), 1)
    own_head = (
        lax.broadcasted_iota(jnp.int32, (kw, vw), 0) // HK
        == lax.broadcasted_iota(jnp.int32, (kw, vw), 1) // HV
    )
    for p in range(channels // kw):
        ks = slice(p * kw, (p + 1) * kw)
        v = values[:, p * vw : (p + 1) * vw]
        s = state[p]
        carried = dot(q_run[:, ks], s.astype(bf16))
        for h in range(group):
            q_head = jnp.where(lane // HK == h, q_mid[:, ks], 0.0).astype(bf16)
            scores = lax.dot_general(
                q_head, k_mid[:, ks], (((1,), (1,)), ((), ())), preferred_element_type=f32
            )
            scores = jnp.where(causal, scores, 0.0).astype(bf16)
            hs = slice(h * HV, (h + 1) * HV)
            first = p * vw + h * HV
            local[:, first : first + HV] = dot(scores, v[:, hs]) + carried[:, hs]
        column = jnp.sum(jnp.where(key_row == key_col, end_decay[:, ks], 0.0), axis=1, keepdims=True)
        added = lax.dot_general(
            k_end[:, ks], v, (((0,), (0,)), ((), ())), preferred_element_type=f32
        )
        state[p] = s * column + jnp.where(own_head, added, 0.0)
    prefix[0:1] = before + end

    @pl.when(step == pl.num_programs(0) - 1)
    def _():
        logs[...] = prefix[0:1]
        for p in range(channels // kw):
            for h in range(group):
                row = p * kw + h * HK
                state_out[row : row + HK] = state[p, h * HK : (h + 1) * HK, h * HV : (h + 1) * HV]


def linear_attention(query, keys, values, pre, bias, extra):
    rows, channels = query.shape
    wide = values.shape[1]
    group = min(2, channels // HK)
    tile = min(BLOCK, rows)
    narrow = pl.BlockSpec((tile, channels), lambda i: (i, 0))
    broad = pl.BlockSpec((tile, wide), lambda i: (i, 0))
    return pl.pallas_call(
        gla_body,
        grid=(rows // tile,),
        in_specs=[narrow, narrow, broad, narrow, whole((1, channels)), narrow],
        out_specs=[broad, narrow, whole((channels, HV)), whole((1, channels))],
        out_shape=[
            jax.ShapeDtypeStruct((rows, wide), f32),
            jax.ShapeDtypeStruct((rows, channels), bf16),
            jax.ShapeDtypeStruct((channels, HV), f32),
            jax.ShapeDtypeStruct((1, channels), f32),
        ],
        scratch_shapes=[
            pltpu.VMEM((channels // HK // group, HK * group, HV * group), f32),
            pltpu.VMEM((8, channels), f32),
        ],
        compiler_params=params(24),
        cost_estimate=pl.CostEstimate(
            flops=20 * rows * tile * wide, bytes_accessed=rows * wide * 8, transcendentals=0
        ),
        name="linear_attention",
    )(query, keys, values, pre, bias, extra)


def mix_body(conv, stats, conv_gain, local, since, state, gate, head_gain, act, *, channels):
    width = conv.shape[1]
    mean_val = stats[:, 0:1] / channels
    square_mean = stats[:, 1:2] / channels
    normal = (conv[...] - mean_val) * lax.rsqrt(square_mean - mean_val * mean_val + epsilon)
    normal = normal * conv_gain[...]
    act[:, :width] = (normal * jax.nn.sigmoid(normal)).astype(bf16)
    keys = since.shape[1]
    group = min(2, keys // HK)
    kw = HK * group
    lane = lax.broadcasted_iota(jnp.int32, (since.shape[0], kw), 1)
    for head in range(keys // HK):
        p, h = divmod(head, group)
        q = jnp.where(lane // HK == h, since[:, p * kw : (p + 1) * kw].astype(f32), 0.0).astype(bf16)
        hs = slice(head * HV, (head + 1) * HV)
        attn = local[:, hs] + dot(q, state[p * kw : (p + 1) * kw].astype(bf16))
        attn = attn * lax.rsqrt(jnp.mean(attn * attn, axis=1, keepdims=True) + epsilon)
        gated = gate[:, hs].astype(f32)
        gated = gated * jax.nn.sigmoid(gated)
        act[:, width + head * HV : width + (head + 1) * HV] = (attn * head_gain[...] * gated).astype(bf16)


def mix(conv, stats, conv_gain, local, since, state, gate, head_gain, channels):
    rows, width = conv.shape
    wide = local.shape[1]
    tile = min(ROW_TILE, rows)

    def tiled(cols):
        return pl.BlockSpec((tile, cols), lambda i: (i, 0))

    return pl.pallas_call(
        functools.partial(mix_body, channels=channels),
        grid=(rows // tile,),
        in_specs=[
            tiled(width),
            tiled(2),
            whole((1, width)),
            tiled(wide),
            tiled(since.shape[1]),
            whole(state.shape),
            tiled(wide),
            whole((1, HV)),
        ],
        out_specs=tiled(width + wide),
        out_shape=jax.ShapeDtypeStruct((rows, width + wide), bf16),
        compiler_params=params(24),
        cost_estimate=pl.CostEstimate(
            flops=8000 * rows * wide, bytes_accessed=rows * wide * 8, transcendentals=0
        ),
        name="mix",
    )(conv, stats, conv_gain, local, since, state, gate, head_gain)


def out_body(offs, act, *refs, pieces):
    weight = refs[-1]
    out = refs[pieces]

    @pl.when(pl.program_id(0) == 0)
    def _():
        for k in range(pieces):
            cols = refs[k].shape[1]
            weight[:, pl.ds(pl.multiple_of(offs[k], cols), cols)] = refs[k][...]

    out[...] = dot(act[...], weight[...]).astype(bf16)


def out_project(act, pieces, offs, total):
    rows, depth = act.shape
    tile = min(ROW_TILE, rows)
    return pl.pallas_call(
        functools.partial(out_body, pieces=len(pieces)),
        grid=(rows // tile,),
        in_specs=[SMEM, pl.BlockSpec((tile, depth), lambda i: (i, 0))]
        + [whole(p.shape) for p in pieces],
        out_specs=pl.BlockSpec((tile, total), lambda i: (i, 0)),
        out_shape=jax.ShapeDtypeStruct((rows, total), bf16),
        scratch_shapes=[pltpu.VMEM((depth, total), bf16)],
        compiler_params=params(36),
        cost_estimate=pl.CostEstimate(
            flops=2 * rows * depth * total, bytes_accessed=rows * total * 2, transcendentals=0
        ),
        name="out_project",
    )(offs, act, *pieces)


def full_features(own, axis):
    if lax.axis_size(axis) != 2:
        return lax.all_gather(own, axis, axis=1, tiled=True)
    other = flip(own, axis, 1)
    low = lax.axis_index(axis) == 0
    return jnp.concatenate([jnp.where(low, own, other), jnp.where(low, other, own)], axis=1)


def normalize(tokens, norm_gain):
    widened = tokens.astype(f32)
    scale = lax.rsqrt(jnp.mean(widened * widened, axis=-1, keepdims=True) + epsilon)
    return (widened * scale * norm_gain).astype(bf16)


def per_device(
    tokens,
    norm_gain,
    w_conv_a,
    w_conv_gate,
    conv_weight,
    conv_gain,
    w_query,
    w_key,
    w_value,
    w_outgate,
    w_decay,
    decay_bias,
    decay_extra,
    head_gain,
    init_state,
    w_out_conv,
    w_out_gla,
):
    rows = tokens.shape[0]
    groups = lax.axis_size("tp")
    width = w_conv_a.shape[1]
    channels = w_query.shape[1]
    wide = w_value.shape[1]

    gla_own = jnp.concatenate([w_query, w_key, w_value, w_decay], axis=1)
    conv_own = jnp.concatenate([w_conv_a, w_conv_gate, w_outgate], axis=1)
    out_own = jnp.concatenate([w_out_conv, w_out_gla], axis=0)
    gla_pieces, gla_offs = gathered(gla_own, "sp", 0, 0)
    conv_pieces, conv_offs = gathered(conv_own, "sp", 0, 1)
    out_pieces, out_offs = gathered(out_own, "sp", 1, 0)

    rim = shifted(tokens[rows - HALO :], "sp", 1)
    normed = normalize(full_features(tokens, "tp"), norm_gain)
    normed_rim = normalize(full_features(rim, "tp"), norm_gain)

    query, keys, values, decay_pre = project(
        normed, gla_pieces, gla_offs, (channels, channels, wide, channels), (bf16, bf16, bf16, f32)
    )
    local, since, end_state, end_logs = linear_attention(
        query, keys, values, decay_pre, decay_bias[None, :], decay_extra
    )
    before_state, before_logs = entering(end_state, end_logs[0], "sp")
    state = before_state + jnp.exp(before_logs)[:, None] * init_state.reshape(channels, HV)

    gated, gate, gated_rim = conv_project(normed, normed_rim, conv_pieces, conv_offs, width, wide)
    conv, sums = convolve(gated, gated_rim, conv_weight)
    stats = sums + flip(sums, "tp", 1) if groups == 2 else lax.psum(sums, "tp")

    act = mix(
        conv, stats, conv_gain[None, :], local, since, state, gate, head_gain[None, :], width * groups
    )
    total = norm_gain.shape[0]
    if groups != 2:
        partial = out_project(act, out_pieces, out_offs, total)
        return lax.psum_scatter(partial, "tp", scatter_dimension=0, tiled=True)
    half = rows // 2
    mine = lax.axis_index("tp")
    theirs = out_project(
        lax.dynamic_slice_in_dim(act, (1 - mine) * half, half), out_pieces, out_offs, total
    )
    received = flip(theirs, "tp", 1)
    kept = out_project(lax.dynamic_slice_in_dim(act, mine * half, half), out_pieces, out_offs, total)
    return (kept.astype(f32) + received.astype(f32)).astype(bf16)


def solution(mesh):
    placed = (
        P("sp", "tp"),
        P(),
        P("sp", "tp"),
        P("sp", "tp"),
        P(None, "tp"),
        P("tp"),
        P("sp", "tp"),
        P("sp", "tp"),
        P("sp", "tp"),
        P("sp", "tp"),
        P("sp", "tp"),
        P("tp"),
        P("sp", "tp"),
        P(),
        P("tp", None, None),
        P("tp", "sp"),
        P("tp", "sp"),
    )
    return jax.shard_map(
        per_device, mesh=mesh, in_specs=placed, out_specs=P(("sp", "tp"), None), check_vma=False
    )
```

```python
import functools

import jax
import jax.numpy as jnp
from jax import lax
from jax.experimental import pallas as pl
from jax.experimental.pallas import tpu as pltpu
from jax.sharding import PartitionSpec as P


HK = 64
HV = 128
BLOCK = 128
LANES = 128
HALO = 32
ROW_TILE = 256
DIRECT = 16


epsilon = 1e-06
gate_divisor = 16.0
f32 = jnp.float32
bf16 = jnp.bfloat16
SMEM = pl.BlockSpec(memory_space=pltpu.SMEM)


def whole(shape):
    return pl.BlockSpec(shape, lambda i: (0,) * len(shape))


def params(megabytes):
    return pltpu.CompilerParams(
        dimension_semantics=("arbitrary",), vmem_limit_bytes=megabytes * 1024 * 1024
    )


def dot(a, b):
    return jnp.dot(a, b, preferred_element_type=f32)


def flip(value, axis, mask):
    count = lax.axis_size(axis)
    pairs = [(i, i ^ mask) for i in range(count)]
    return lax.ppermute(value, axis, pairs)


def is_middle(place):
    return (place >> 2 ^ place >> 3) & 1


def exchange(value, axis):
    count = lax.axis_size(axis)
    pairs = [(i, i ^ 12) for i in range(count) if is_middle(i)]
    return lax.ppermute(value, axis, pairs)


def hand_on(value, axis):
    count = lax.axis_size(axis)
    pairs = [(i, i ^ 4) for i in range(count) if is_middle(i)]
    return lax.ppermute(value, axis, pairs)


def chosen(axis, dim, *options):
    flag = is_middle(lax.axis_index(axis)).astype(jnp.int32).reshape(1)
    return choose(flag, options, dim)


def relayed(own, axis, dim):
    def send(value, mask):
        return flip(value, axis, mask)

    na = exchange(own, axis)
    z1 = send(own, 4)
    x0 = send(own, 1)
    y0 = send(own, 2)
    fa = hand_on(na, axis)
    nb = exchange(z1, axis)
    x1 = send(z1, 1)
    y1 = send(z1, 2)
    d0 = send(y0, 1)
    a0 = chosen(axis, dim, (na, fa))
    fb = hand_on(nb, axis)
    xa = send(a0, 1)
    ya = send(a0, 2)
    d1 = send(x1, 2)
    b0 = chosen(axis, dim, (nb, fb))
    xb = send(b0, 1)
    yb = send(b0, 2)
    da = send(ya, 1)
    db = send(xb, 2)
    order = [own, x0, y0, d0, z1, x1, y1, d1] + [None] * 8 + [a0, xa, ya, da, b0, xb, yb, db]
    return [(piece, (place,)) for place, piece in enumerate(order) if piece is not None]


def doubled(own, axis, dim, turn):
    first, second = (2, 1) if turn else (1, 2)

    def send(value, mask):
        return flip(value, axis, mask)

    z1 = send(own, 4)
    na = exchange(own, axis)
    nb = exchange(z1, axis)
    fa = hand_on(na, axis)
    fb = hand_on(nb, axis)
    x0 = send(own, first)
    pair = chosen(axis, dim, (own, own), (z1, z1))
    far = chosen(axis, dim, (na, fa), (nb, fb))
    yp = send(pair, second)
    x1 = send(x0, 4)
    dp = send(yp, first)
    xq = send(far, first)
    yq = send(far, second)
    dq = send(xq, second)

    def nears(place):
        return (place, place | 4)

    def fars(place):
        return (16 + place, 20 + place)

    return [
        (pair, nears(0)),
        (x0, (first,)),
        (x1, (first | 4,)),
        (yp, nears(second)),
        (dp, nears(3)),
        (far, fars(0)),
        (xq, fars(first)),
        (yq, fars(second)),
        (dq, fars(3)),
    ]


def spread(own, axis, dim, turn, plan):
    count = lax.axis_size(axis)
    if count == DIRECT:
        if plan == "single":
            return relayed(own, axis, dim)
        return doubled(own, axis, dim, turn)
    pieces = {0: own}
    mask = 1
    while mask < count:
        for place in list(pieces):
            pieces[place | mask] = flip(pieces[place], axis, mask)
        mask *= 2
    return [(piece, (place,)) for place, piece in pieces.items()]


def gathered(own, axis, dim, turn, plan):
    count = lax.axis_size(axis)
    if count > DIRECT or count & (count - 1):
        pieces = [(lax.all_gather(own, axis, axis=dim, tiled=True), (0,))]
        offs = jnp.zeros((1,), jnp.int32)
    else:
        pieces = spread(own, axis, dim, turn, plan)
        place = lax.axis_index(axis)
        order = jnp.arange(count, dtype=jnp.int32)
        turned = 4 * is_middle(place)
        near = jnp.arange(4, dtype=jnp.int32)
        order = jnp.concatenate([order, near ^ 8 ^ turned, near ^ 12 ^ turned])
        offs = (order ^ place) * own.shape[dim]
    return [p for p, _ in pieces], tuple(q for _, q in pieces), offs


def shifted(value, axis, steps):
    count = lax.axis_size(axis)
    return lax.ppermute(value, axis, [(i, i + steps) for i in range(count - steps)])


def entering(held, packed, axis):
    place = lax.axis_index(axis)
    bits = lax.axis_size(axis).bit_length() - 1
    for bit in range(bits):
        upper = ((place >> bit) & 1).astype(jnp.int32).reshape(1)
        received = flip(packed, axis, 1 << bit)
        if bit + 1 == bits:
            return held, received, upper
        held, packed = combine(upper, received, held)


def choose_body(flag, *refs, dim):
    out, sem = refs[-2:]
    ins = refs[:-2]
    for number, middle in enumerate((True, False)):
        picked = [pair[number] for pair in zip(ins[::2], ins[1::2])]

        @pl.when((flag[0] == 1) == middle)
        def _():
            copies = []
            start = 0
            for k, ref in enumerate(picked):
                there = pl.ds(start, ref.shape[dim])
                target = out.at[:, there] if dim else out.at[there, :]
                copies.append(pltpu.make_async_copy(ref, target, sem.at[k]))
                start += ref.shape[dim]
            for copy in copies:
                copy.start()
            for copy in copies:
                copy.wait()


def choose(flag, options, dim):
    shape = list(options[0][0].shape)
    shape[dim] = sum(first.shape[dim] for first, _ in options)
    flat = [array for pair in options for array in pair]
    vmem = pl.BlockSpec(memory_space=pltpu.VMEM)
    return pl.pallas_call(
        functools.partial(choose_body, dim=dim),
        in_specs=[SMEM] + [vmem] * len(flat),
        out_specs=vmem,
        out_shape=jax.ShapeDtypeStruct(tuple(shape), flat[0].dtype),
        scratch_shapes=[pltpu.SemaphoreType.DMA((len(options),))],
        compiler_params=pltpu.CompilerParams(vmem_limit_bytes=2 * 1024 * 1024),
        name="choose",
    )(flag, *flat)


def norm_body(places, *refs):
    *ins, gain, out = refs
    total = None
    for ref in ins:
        wide = ref[...].astype(f32)
        part = jnp.sum(wide * wide, axis=1, keepdims=True)
        total = part if total is None else total + part
    scale = lax.rsqrt(total / out.shape[1] + epsilon)
    for k, ref in enumerate(ins):
        cols = pl.ds(pl.multiple_of(places[k], LANES), ref.shape[1])
        out[:, cols] = (ref[...].astype(f32) * scale * gain[0:1, cols]).astype(bf16)


def normalize(parts, places, gain):
    rows, total = parts[0].shape[0], gain.shape[0]
    tile = min(ROW_TILE, rows)
    return pl.pallas_call(
        norm_body,
        grid=(rows // tile,),
        in_specs=[SMEM]
        + [pl.BlockSpec((tile, p.shape[1]), lambda i: (i, 0)) for p in parts]
        + [whole((1, total))],
        out_specs=pl.BlockSpec((tile, total), lambda i: (i, 0)),
        out_shape=jax.ShapeDtypeStruct((rows, total), bf16),
        compiler_params=params(58),
        name="normalize",
    )(places, *parts, gain[None, :])


def place_pieces(offs, refs, weight, places, dim):
    for ref, spots in zip(refs, places):
        size = ref.shape[dim] // len(spots)
        for k, spot in enumerate(spots):
            there = pl.ds(pl.multiple_of(offs[spot], size), size)
            here = slice(k * size, (k + 1) * size)
            if dim:
                weight[:, there] = ref[:, here]
            else:
                weight[there, :] = ref[here, :]


def project_body(offs, normed, *refs, places):
    weight = refs[-1]
    outs = refs[len(places) : -1]

    @pl.when(pl.program_id(0) == 0)
    def _():
        place_pieces(offs, refs, weight, places, 0)

    start = 0
    for out in outs:
        width = out.shape[1]
        out[...] = dot(normed[...], weight[:, start : start + width]).astype(out.dtype)
        start += width


def project(normed, pieces, places, offs, widths, kinds):
    rows, depth = normed.shape
    total = sum(widths)
    tile = min(ROW_TILE, rows)
    return pl.pallas_call(
        functools.partial(project_body, places=places),
        grid=(rows // tile,),
        in_specs=[SMEM, pl.BlockSpec((tile, depth), lambda i: (i, 0))]
        + [whole(p.shape) for p in pieces],
        out_specs=[pl.BlockSpec((tile, w), lambda i: (i, 0)) for w in widths],
        out_shape=[jax.ShapeDtypeStruct((rows, w), k) for w, k in zip(widths, kinds)],
        scratch_shapes=[pltpu.VMEM((depth, total), bf16)],
        compiler_params=params(58),
        cost_estimate=pl.CostEstimate(
            flops=2 * rows * depth * total, bytes_accessed=rows * depth * 2, transcendentals=0
        ),
        name="project",
    )(offs, normed, *pieces)


def conv_project_body(offs, normed, before, *refs, places):
    weight = refs[-1]
    gated, gate_out, rim = refs[len(places) : -1]
    width = gated.shape[1]

    def gate(values):
        left = values[:, :width].astype(bf16).astype(f32)
        right = values[:, width : 2 * width].astype(bf16).astype(f32)
        return (left * jax.nn.sigmoid(right)).astype(bf16)

    @pl.when(pl.program_id(0) == 0)
    def _():
        place_pieces(offs, refs, weight, places, 0)
        rim[...] = gate(dot(before[...], weight[:, : 2 * width]))

    gated[...] = gate(dot(normed[...], weight[:, : 2 * width]))
    gate_out[...] = dot(normed[...], weight[:, 2 * width :]).astype(bf16)


def conv_project(normed, before, pieces, places, offs, width, gate_width):
    rows, depth = normed.shape
    total = 2 * width + gate_width
    tile = min(ROW_TILE, rows)
    return pl.pallas_call(
        functools.partial(conv_project_body, places=places),
        grid=(rows // tile,),
        in_specs=[SMEM, pl.BlockSpec((tile, depth), lambda i: (i, 0)), whole(before.shape)]
        + [whole(p.shape) for p in pieces],
        out_specs=[
            pl.BlockSpec((tile, width), lambda i: (i, 0)),
            pl.BlockSpec((tile, gate_width), lambda i: (i, 0)),
            whole((before.shape[0], width)),
        ],
        out_shape=[
            jax.ShapeDtypeStruct((rows, width), bf16),
            jax.ShapeDtypeStruct((rows, gate_width), bf16),
            jax.ShapeDtypeStruct((before.shape[0], width), bf16),
        ],
        scratch_shapes=[pltpu.VMEM((depth, total), bf16)],
        compiler_params=params(58),
        cost_estimate=pl.CostEstimate(
            flops=2 * rows * depth * total, bytes_accessed=rows * depth * 2, transcendentals=0
        ),
        name="conv_project",
    )(offs, normed, before, *pieces)


def conv_body(gated, rim, taps, out, sums, extended):
    rows, width = gated.shape
    count = taps.shape[0]
    first = HALO - count + 1
    chunk = 64
    extended[:HALO] = rim[...].astype(f32)
    extended[HALO : HALO + rows] = gated[...].astype(f32)
    extended[HALO + rows :] = jnp.zeros((8, width), f32)

    def step(i, carry):
        base = pl.multiple_of(i * chunk, chunk)
        there = pl.ds(base, chunk)
        total = jnp.zeros((chunk, LANES), f32)
        square = jnp.zeros((chunk, LANES), f32)
        for lane in range(0, width, LANES):
            here = slice(lane, lane + LANES)
            near = extended[pl.ds(base, chunk + HALO + 8), here]
            result = None
            for residue in range(8):
                acc = None
                for start in range(0, HALO + 1, 8):
                    tap = start + residue - first
                    if 0 <= tap < count:
                        part = taps[tap : tap + 1, here] * near[start : start + chunk + 8]
                        acc = part if acc is None else acc + part
                if residue:
                    acc = pltpu.roll(acc, chunk + 8 - residue, 0)
                acc = acc[:chunk]
                result = acc if result is None else result + acc
            out[there, here] = result.astype(bf16)
            total = total + result
            square = square + result * result
        sums[there, 0:1] = jnp.sum(total, axis=1, keepdims=True)
        sums[there, 1:2] = jnp.sum(square, axis=1, keepdims=True)
        return carry

    lax.fori_loop(0, rows // chunk, step, 0)


def convolve(gated, rim, taps):
    rows, width = gated.shape
    return pl.pallas_call(
        conv_body,
        out_shape=[
            jax.ShapeDtypeStruct((rows, width), bf16),
            jax.ShapeDtypeStruct((rows, 2), f32),
        ],
        scratch_shapes=[
            pltpu.VMEM((HALO + rows + 8, width), f32),
        ],
        compiler_params=pltpu.CompilerParams(vmem_limit_bytes=58 * 1024 * 1024),
        cost_estimate=pl.CostEstimate(
            flops=20 * rows * width * taps.shape[0], bytes_accessed=rows * width * 6, transcendentals=0
        ),
        name="convolve",
    )(gated, rim, taps)


def gla_body(query, keys, values, pre, bias, extra, local, since, held, packed, state, prefix):
    rows, channels = query.shape
    step = pl.program_id(0)
    group = min(2, channels // HK)
    kw, vw = HK * group, HV * group

    @pl.when(step == 0)
    def _():
        state[...] = jnp.zeros(state.shape, f32)
        prefix[...] = jnp.zeros(prefix.shape, f32)

    biased = pre[...] + bias[...]
    log_decay = (jnp.minimum(biased, 0.0) - jnp.log1p(jnp.exp(-jnp.abs(biased)))) / gate_divisor
    log_decay = log_decay + extra[...]
    at = lax.broadcasted_iota(jnp.int32, (rows, rows), 0)
    by = lax.broadcasted_iota(jnp.int32, (rows, rows), 1)
    causal = at >= by
    cum = jnp.dot(
        causal.astype(f32), log_decay, preferred_element_type=f32, precision=lax.Precision.HIGHEST
    )
    middle = cum[rows // 2 - 1 : rows // 2]
    end = cum[rows - 1 : rows]
    before = prefix[0:1]
    q = query[...].astype(f32) * HK ** (-0.5)
    k = keys[...].astype(f32)
    grown = jnp.exp(cum)
    q_mid = q * jnp.exp(cum - middle)
    k_mid = (k * jnp.exp(middle - cum)).astype(bf16)
    k_end = (k * jnp.exp(end - cum)).astype(bf16)
    q_run = q * grown
    since[...] = (q_run * jnp.exp(before)).astype(bf16)
    q_run = q_run.astype(bf16)
    end_decay = jnp.exp(end)
    key_row = lax.broadcasted_iota(jnp.int32, (kw, kw), 0)
    key_col = lax.broadcasted_iota(jnp.int32, (kw, kw), 1)
    lane = lax.broadcasted_iota(jnp.int32, (rows, kw), 1)
    own_head = (
        lax.broadcasted_iota(jnp.int32, (kw, vw), 0) // HK
        == lax.broadcasted_iota(jnp.int32, (kw, vw), 1) // HV
    )
    for p in range(channels // kw):
        ks = slice(p * kw, (p + 1) * kw)
        v = values[:, p * vw : (p + 1) * vw]
        s = state[p]
        carried = dot(q_run[:, ks], s.astype(bf16))
        for h in range(group):
            q_head = jnp.where(lane // HK == h, q_mid[:, ks], 0.0).astype(bf16)
            scores = lax.dot_general(
                q_head, k_mid[:, ks], (((1,), (1,)), ((), ())), preferred_element_type=f32
            )
            scores = jnp.where(causal, scores, 0.0).astype(bf16)
            hs = slice(h * HV, (h + 1) * HV)
            first = p * vw + h * HV
            local[:, first : first + HV] = (dot(scores, v[:, hs]) + carried[:, hs]).astype(bf16)
        column = jnp.sum(jnp.where(key_row == key_col, end_decay[:, ks], 0.0), axis=1, keepdims=True)
        added = lax.dot_general(
            k_end[:, ks], v, (((0,), (0,)), ((), ())), preferred_element_type=f32
        )
        state[p] = s * column + jnp.where(own_head, added, 0.0)
    prefix[0:1] = before + end

    @pl.when(step == pl.num_programs(0) - 1)
    def _():
        everything = prefix[0:1]
        for p in range(channels // kw):
            column = jnp.sum(
                jnp.where(key_row == key_col, everything[:, p * kw : (p + 1) * kw], 0.0), axis=1, keepdims=True
            )
            held[p * kw : (p + 1) * kw, 3 * HV :] = jnp.broadcast_to(column, (kw, HV))
            for h in range(group):
                row = p * kw + h * HK
                own = state[p, h * HK : (h + 1) * HK, h * HV : (h + 1) * HV]
                held[row : row + HK, 2 * HV : 3 * HV] = own
        held[:, : 2 * HV] = jnp.zeros((channels, 2 * HV), f32)
        packed[:, :HV], packed[:, HV:] = packing(held[:, 2 * HV : 3 * HV], held[:, 3 * HV :])


def linear_attention(query, keys, values, pre, bias, extra):
    rows, channels = query.shape
    wide = values.shape[1]
    group = min(2, channels // HK)
    tile = min(BLOCK, rows)
    narrow = pl.BlockSpec((tile, channels), lambda i: (i, 0))
    broad = pl.BlockSpec((tile, wide), lambda i: (i, 0))
    return pl.pallas_call(
        gla_body,
        grid=(rows // tile,),
        in_specs=[narrow, narrow, broad, narrow, whole((1, channels)), narrow],
        out_specs=[broad, narrow, whole((channels, 4 * HV)), whole((channels, 2 * HV))],
        out_shape=[
            jax.ShapeDtypeStruct((rows, wide), bf16),
            jax.ShapeDtypeStruct((rows, channels), bf16),
            jax.ShapeDtypeStruct((channels, 4 * HV), f32),
            jax.ShapeDtypeStruct((channels, 2 * HV), bf16),
        ],
        scratch_shapes=[
            pltpu.VMEM((channels // HK // group, HK * group, HV * group), f32),
            pltpu.VMEM((8, channels), f32),
        ],
        compiler_params=params(24),
        cost_estimate=pl.CostEstimate(
            flops=20 * rows * tile * wide, bytes_accessed=rows * wide * 8, transcendentals=0
        ),
        name="linear_attention",
    )(query, keys, values, pre, bias, extra)


def packing(state, logs):
    high = logs.astype(bf16)
    lane = lax.broadcasted_iota(jnp.int32, logs.shape, 1)
    low = (logs - high.astype(f32)).astype(bf16)
    return state.astype(bf16), jnp.where(lane < HV // 2, high.astype(f32), low.astype(f32)).astype(bf16)


def unpacking(packed):
    half = packed[:, HV : 2 * HV].astype(f32)
    logs = half[:, 0:1] + half[:, HV // 2 : HV // 2 + 1]
    return packed[:, :HV].astype(f32), jnp.broadcast_to(logs, half.shape)


def combine_body(upper, packed, held, held_out, packed_out):
    state, logs = unpacking(packed)
    above = upper[0] == 1
    pre, pre_logs, own, own_logs = (held[:, k * HV : (k + 1) * HV] for k in range(4))
    held_out[:, :HV] = jnp.where(above, jnp.exp(pre_logs) * state + pre, pre)
    held_out[:, HV : 2 * HV] = jnp.where(above, pre_logs + logs, pre_logs)
    joined = jnp.where(above, jnp.exp(own_logs) * state + own, jnp.exp(logs) * own + state)
    joined_logs = own_logs + logs
    held_out[:, 2 * HV : 3 * HV] = joined
    held_out[:, 3 * HV :] = joined_logs
    packed_out[:, :HV], packed_out[:, HV:] = packing(joined, joined_logs)


def combine(upper, packed, held):
    vmem = pl.BlockSpec(memory_space=pltpu.VMEM)
    return pl.pallas_call(
        combine_body,
        in_specs=[SMEM, vmem, vmem],
        out_specs=[vmem, vmem],
        out_shape=[
            jax.ShapeDtypeStruct(held.shape, f32),
            jax.ShapeDtypeStruct(packed.shape, bf16),
        ],
        compiler_params=pltpu.CompilerParams(vmem_limit_bytes=4 * 1024 * 1024),
        name="combine",
    )(upper, packed, held)


def finish_body(start, offs, *refs, channels, parts, places):
    sums, refs = refs[:parts], refs[parts:]
    conv, conv_gain, local, since, upper, packed, held, init, gate, head_gain, *refs = refs
    weights, (out, state, act) = refs[: len(places)], refs[len(places) :]

    @pl.when(pl.program_id(0) == 0)
    def _():
        last, logs = unpacking(packed)
        above = upper[0] == 1
        pre, pre_logs = held[:, :HV], held[:, HV : 2 * HV]
        started = jnp.where(above, jnp.exp(pre_logs) * last + pre, pre)
        logs = jnp.where(above, pre_logs + logs, pre_logs)
        state[...] = (started + jnp.exp(logs) * init[...]).astype(bf16)

    width = conv.shape[1]
    stats = sums[0][...]
    for more in sums[1:]:
        stats = stats + more[...]
    mean_val = stats[:, 0:1] / channels
    square_mean = stats[:, 1:2] / channels
    normal = (conv[...].astype(f32) - mean_val) * lax.rsqrt(square_mean - mean_val * mean_val + epsilon)
    normal = normal * conv_gain[...]
    act[:, :width] = (normal * jax.nn.sigmoid(normal)).astype(bf16)
    keys = since.shape[1]
    group = min(2, keys // HK)
    kw = HK * group
    lane = lax.broadcasted_iota(jnp.int32, (since.shape[0], kw), 1)
    for head in range(keys // HK):
        p, h = divmod(head, group)
        q = jnp.where(lane // HK == h, since[:, p * kw : (p + 1) * kw].astype(f32), 0.0).astype(bf16)
        hs = slice(head * HV, (head + 1) * HV)
        attn = local[:, hs].astype(f32) + dot(q, state[p * kw : (p + 1) * kw])
        attn = attn * lax.rsqrt(jnp.mean(attn * attn, axis=1, keepdims=True) + epsilon)
        gated = gate[:, hs].astype(f32)
        gated = gated * jax.nn.sigmoid(gated)
        act[:, width + head * HV : width + (head + 1) * HV] = (attn * head_gain[...] * gated).astype(bf16)
    for ref, spots in zip(weights, places):
        size = ref.shape[1] // len(spots)
        values = dot(act[...], ref[...]).astype(bf16)
        for k, spot in enumerate(spots):
            there = pl.ds(pl.multiple_of(offs[spot], size), size)
            out[:, there] = values[:, k * size : (k + 1) * size]


def finish(first, rows, sums, conv, conv_gain, local, since, before, init, gate, head_gain, out_weights, total, channels):
    pieces, places, offs = out_weights
    width, wide = conv.shape[1], local.shape[1]
    tile = min(ROW_TILE, rows)
    held, packed, upper = before
    start = (first // tile).astype(jnp.int32).reshape(1)

    def tiled(cols):
        return pl.BlockSpec((tile, cols), lambda i, at: (at[0] + i, 0))

    def fixed(shape):
        return pl.BlockSpec(shape, lambda i, at: (0, 0))

    spec = pltpu.PrefetchScalarGridSpec(
        num_scalar_prefetch=1,
        grid=(rows // tile,),
        in_specs=[SMEM]
        + [tiled(2) for _ in sums]
        + [
            tiled(width),
            fixed((1, width)),
            tiled(wide),
            tiled(since.shape[1]),
            SMEM,
            fixed(packed.shape),
            fixed(held.shape),
            fixed(init.shape),
            tiled(wide),
            fixed((1, HV)),
        ]
        + [pl.BlockSpec(memory_space=pltpu.VMEM) for _ in pieces],
        out_specs=pl.BlockSpec((tile, total), lambda i, at: (i, 0)),
        scratch_shapes=[pltpu.VMEM(init.shape, bf16), pltpu.VMEM((tile, width + wide), bf16)],
    )
    return pl.pallas_call(
        functools.partial(finish_body, channels=channels, parts=len(sums), places=places),
        grid_spec=spec,
        out_shape=jax.ShapeDtypeStruct((rows, total), bf16),
        compiler_params=params(56),
        cost_estimate=pl.CostEstimate(
            flops=2 * rows * (width + wide) * total, bytes_accessed=rows * total * 2, transcendentals=0
        ),
        name="finish",
    )(start, offs, *sums, conv, conv_gain, local, since, upper, packed, held, init, gate, head_gain, *pieces)


def normed_rows(own, axis, norm_gain):
    if lax.axis_size(axis) != 2:
        full = lax.all_gather(own, axis, axis=1, tiled=True)
        return normalize([full], jnp.zeros((1,), jnp.int32), norm_gain)
    other = flip(own, axis, 1)
    mine = lax.axis_index(axis)
    places = jnp.stack([mine, 1 - mine]).astype(jnp.int32) * own.shape[1]
    return normalize([own, other], places, norm_gain)


def per_device(
    tokens,
    norm_gain,
    w_conv_a,
    w_conv_gate,
    conv_weight,
    conv_gain,
    w_query,
    w_key,
    w_value,
    w_outgate,
    w_decay,
    decay_bias,
    decay_extra,
    head_gain,
    init_state,
    w_out_conv,
    w_out_gla,
):
    rows = tokens.shape[0]
    groups = lax.axis_size("tp")
    width = w_conv_a.shape[1]
    channels = w_query.shape[1]
    wide = w_value.shape[1]

    gla_own = jnp.concatenate([w_query, w_key, w_value, w_decay], axis=1)
    conv_own = jnp.concatenate([w_conv_a, w_conv_gate, w_outgate], axis=1)
    out_own = jnp.concatenate([w_out_conv, w_out_gla], axis=0)
    gla_weights = gathered(gla_own, "sp", 0, 0, "single")
    conv_weights = gathered(conv_own, "sp", 0, 0, "double")
    out_weights = gathered(out_own, "sp", 1, 1, "double")

    rim = shifted(tokens[rows - HALO :], "sp", 1)
    normed = normed_rows(tokens, "tp", norm_gain)
    normed_rim = normed_rows(rim, "tp", norm_gain)

    query, keys, values, decay_pre = project(
        normed, *gla_weights, (channels, channels, wide, channels), (bf16, bf16, bf16, f32)
    )
    local, since, *end = linear_attention(
        query, keys, values, decay_pre, decay_bias[None, :], decay_extra
    )
    before = entering(*end, "sp")

    gated, gate, gated_rim = conv_project(normed, normed_rim, *conv_weights, width, wide)
    conv, sums = convolve(gated, gated_rim, conv_weight)
    sums = [sums, flip(sums, "tp", 1)] if groups == 2 else [lax.psum(sums, "tp")]

    init = init_state.reshape(channels, HV)
    total = norm_gain.shape[0]

    def rows_from(first, count):
        return finish(
            jnp.asarray(first),
            count,
            sums,
            conv,
            conv_gain[None, :],
            local,
            since,
            before,
            init,
            gate,
            head_gain[None, :],
            out_weights,
            total,
            width * groups,
        )

    if groups != 2:
        return lax.psum_scatter(rows_from(0, rows), "tp", scatter_dimension=0, tiled=True)
    half = rows // 2
    mine = lax.axis_index("tp")
    received = flip(rows_from((1 - mine) * half, half), "tp", 1)
    kept = rows_from(mine * half, half)
    return (kept.astype(f32) + received.astype(f32)).astype(bf16)


def solution(mesh):
    placed = (
        P("sp", "tp"),
        P(),
        P("sp", "tp"),
        P("sp", "tp"),
        P(None, "tp"),
        P("tp"),
        P("sp", "tp"),
        P("sp", "tp"),
        P("sp", "tp"),
        P("sp", "tp"),
        P("sp", "tp"),
        P("tp"),
        P("sp", "tp"),
        P(),
        P("tp", None, None),
        P("tp", "sp"),
        P("tp", "sp"),
    )

    return jax.shard_map(
        per_device, mesh=mesh, in_specs=placed, out_specs=P(("sp", "tp"), None), check_vma=False
    )
```

```python
import functools

import jax
import jax.numpy as jnp
from jax import lax
from jax.experimental import pallas as pl
from jax.experimental.pallas import tpu as pltpu
from jax.sharding import PartitionSpec as P


HK = 64
HV = 128
BLOCK = 128
LANES = 128
HALO = 32
ROW_TILE = 256
DIRECT = 16


epsilon = 1e-06
gate_divisor = 16.0
f32 = jnp.float32
bf16 = jnp.bfloat16
SMEM = pl.BlockSpec(memory_space=pltpu.SMEM)


def whole(shape):
    return pl.BlockSpec(shape, lambda i: (0,) * len(shape))


def params(megabytes):
    return pltpu.CompilerParams(
        dimension_semantics=("arbitrary",), vmem_limit_bytes=megabytes * 1024 * 1024
    )


def dot(a, b):
    return jnp.dot(a, b, preferred_element_type=f32)


def flip(value, axis, mask):
    count = lax.axis_size(axis)
    pairs = [(i, i ^ mask) for i in range(count)]
    return lax.ppermute(value, axis, pairs)


def is_middle(place):
    return (place >> 2 ^ place >> 3) & 1


def exchange(value, axis):
    count = lax.axis_size(axis)
    pairs = [(i, i ^ 12) for i in range(count) if is_middle(i)]
    return lax.ppermute(value, axis, pairs)


def hand_on(value, axis):
    count = lax.axis_size(axis)
    pairs = [(i, i ^ 4) for i in range(count) if is_middle(i)]
    return lax.ppermute(value, axis, pairs)


def chosen(axis, dim, *options):
    flag = is_middle(lax.axis_index(axis)).astype(jnp.int32).reshape(1)
    return choose(flag, options, dim)


def relayed(own, axis, dim):
    def send(value, mask):
        return flip(value, axis, mask)

    na = exchange(own, axis)
    z1 = send(own, 4)
    x0 = send(own, 1)
    y0 = send(own, 2)
    fa = hand_on(na, axis)
    nb = exchange(z1, axis)
    x1 = send(z1, 1)
    y1 = send(z1, 2)
    d0 = send(y0, 1)
    a0 = chosen(axis, dim, (na, fa))
    fb = hand_on(nb, axis)
    xa = send(a0, 1)
    ya = send(a0, 2)
    d1 = send(x1, 2)
    b0 = chosen(axis, dim, (nb, fb))
    xb = send(b0, 1)
    yb = send(b0, 2)
    da = send(ya, 1)
    db = send(xb, 2)
    order = [own, x0, y0, d0, z1, x1, y1, d1] + [None] * 8 + [a0, xa, ya, da, b0, xb, yb, db]
    return [(piece, (place,)) for place, piece in enumerate(order) if piece is not None]


def doubled(own, axis, dim, turn):
    first, second = (2, 1) if turn else (1, 2)

    def send(value, mask):
        return flip(value, axis, mask)

    z1 = send(own, 4)
    na = exchange(own, axis)
    nb = exchange(z1, axis)
    fa = hand_on(na, axis)
    fb = hand_on(nb, axis)
    x0 = send(own, first)
    pair = chosen(axis, dim, (own, own), (z1, z1))
    far = chosen(axis, dim, (na, fa), (nb, fb))
    yp = send(pair, second)
    x1 = send(x0, 4)
    dp = send(yp, first)
    xq = send(far, first)
    yq = send(far, second)
    dq = send(xq, second)

    def nears(place):
        return (place, place | 4)

    def fars(place):
        return (16 + place, 20 + place)

    return [
        (pair, nears(0)),
        (x0, (first,)),
        (x1, (first | 4,)),
        (yp, nears(second)),
        (dp, nears(3)),
        (far, fars(0)),
        (xq, fars(first)),
        (yq, fars(second)),
        (dq, fars(3)),
    ]


def spread(own, axis, dim, turn, plan):
    count = lax.axis_size(axis)
    if count == DIRECT:
        if plan == "single":
            return relayed(own, axis, dim)
        return doubled(own, axis, dim, turn)
    pieces = {0: own}
    mask = 1
    while mask < count:
        for place in list(pieces):
            pieces[place | mask] = flip(pieces[place], axis, mask)
        mask *= 2
    return [(piece, (place,)) for place, piece in pieces.items()]


def gathered(own, axis, dim, turn, plan):
    count = lax.axis_size(axis)
    if count > DIRECT or count & (count - 1):
        pieces = [(lax.all_gather(own, axis, axis=dim, tiled=True), (0,))]
        offs = jnp.zeros((1,), jnp.int32)
    else:
        pieces = spread(own, axis, dim, turn, plan)
        place = lax.axis_index(axis)
        order = jnp.arange(count, dtype=jnp.int32)
        turned = 4 * is_middle(place)
        near = jnp.arange(4, dtype=jnp.int32)
        order = jnp.concatenate([order, near ^ 8 ^ turned, near ^ 12 ^ turned])
        offs = (order ^ place) * own.shape[dim]
    return [p for p, _ in pieces], tuple(q for _, q in pieces), offs


def shifted(value, axis, steps):
    count = lax.axis_size(axis)
    return lax.ppermute(value, axis, [(i, i + steps) for i in range(count - steps)])


def entering(held, packed, axis):
    place = lax.axis_index(axis)
    bits = lax.axis_size(axis).bit_length() - 1
    for bit in range(bits):
        upper = ((place >> bit) & 1).astype(jnp.int32).reshape(1)
        received = flip(packed, axis, 1 << bit)
        if bit + 1 == bits:
            return held, received, upper
        held, packed = combine(upper, received, held)


def choose_body(flag, *refs, dim):
    out, sem = refs[-2:]
    ins = refs[:-2]
    for number, middle in enumerate((True, False)):
        picked = [pair[number] for pair in zip(ins[::2], ins[1::2])]

        @pl.when((flag[0] == 1) == middle)
        def _():
            copies = []
            start = 0
            for k, ref in enumerate(picked):
                there = pl.ds(start, ref.shape[dim])
                target = out.at[:, there] if dim else out.at[there, :]
                copies.append(pltpu.make_async_copy(ref, target, sem.at[k]))
                start += ref.shape[dim]
            for copy in copies:
                copy.start()
            for copy in copies:
                copy.wait()


def choose(flag, options, dim):
    shape = list(options[0][0].shape)
    shape[dim] = sum(first.shape[dim] for first, _ in options)
    flat = [array for pair in options for array in pair]
    vmem = pl.BlockSpec(memory_space=pltpu.VMEM)
    return pl.pallas_call(
        functools.partial(choose_body, dim=dim),
        in_specs=[SMEM] + [vmem] * len(flat),
        out_specs=vmem,
        out_shape=jax.ShapeDtypeStruct(tuple(shape), flat[0].dtype),
        scratch_shapes=[pltpu.SemaphoreType.DMA((len(options),))],
        compiler_params=pltpu.CompilerParams(vmem_limit_bytes=2 * 1024 * 1024),
        name="choose",
    )(flag, *flat)


def norm_body(places, *refs):
    *ins, gain, out = refs
    total = None
    for ref in ins:
        wide = ref[...].astype(f32)
        part = jnp.sum(wide * wide, axis=1, keepdims=True)
        total = part if total is None else total + part
    scale = lax.rsqrt(total / out.shape[1] + epsilon)
    for k, ref in enumerate(ins):
        cols = pl.ds(pl.multiple_of(places[k], LANES), ref.shape[1])
        out[:, cols] = (ref[...].astype(f32) * scale * gain[0:1, cols]).astype(bf16)


def normalize(parts, places, gain):
    rows, total = parts[0].shape[0], gain.shape[0]
    tile = min(ROW_TILE, rows)
    return pl.pallas_call(
        norm_body,
        grid=(rows // tile,),
        in_specs=[SMEM]
        + [pl.BlockSpec((tile, p.shape[1]), lambda i: (i, 0)) for p in parts]
        + [whole((1, total))],
        out_specs=pl.BlockSpec((tile, total), lambda i: (i, 0)),
        out_shape=jax.ShapeDtypeStruct((rows, total), bf16),
        compiler_params=params(58),
        name="normalize",
    )(places, *parts, gain[None, :])


def place_pieces(offs, refs, weight, places, dim):
    for ref, spots in zip(refs, places):
        size = ref.shape[dim] // len(spots)
        for k, spot in enumerate(spots):
            there = pl.ds(pl.multiple_of(offs[spot], size), size)
            here = slice(k * size, (k + 1) * size)
            if dim:
                weight[:, there] = ref[:, here]
            else:
                weight[there, :] = ref[here, :]


def project_body(offs, normed, *refs, places):
    weight = refs[-1]
    outs = refs[len(places) : -1]

    @pl.when(pl.program_id(0) == 0)
    def _():
        place_pieces(offs, refs, weight, places, 0)

    start = 0
    for out in outs:
        width = out.shape[1]
        out[...] = dot(normed[...], weight[:, start : start + width]).astype(out.dtype)
        start += width


def project(normed, pieces, places, offs, widths, kinds):
    rows, depth = normed.shape
    total = sum(widths)
    tile = min(ROW_TILE, rows)
    return pl.pallas_call(
        functools.partial(project_body, places=places),
        grid=(rows // tile,),
        in_specs=[SMEM, pl.BlockSpec((tile, depth), lambda i: (i, 0))]
        + [whole(p.shape) for p in pieces],
        out_specs=[pl.BlockSpec((tile, w), lambda i: (i, 0)) for w in widths],
        out_shape=[jax.ShapeDtypeStruct((rows, w), k) for w, k in zip(widths, kinds)],
        scratch_shapes=[pltpu.VMEM((depth, total), bf16)],
        compiler_params=params(58),
        cost_estimate=pl.CostEstimate(
            flops=2 * rows * depth * total, bytes_accessed=rows * depth * 2, transcendentals=0
        ),
        name="project",
    )(offs, normed, *pieces)


def conv_project_body(offs, normed, before, *refs, places):
    weight = refs[-1]
    gated, gate_out, rim = refs[len(places) : -1]
    width = gated.shape[1]

    def gate(values):
        left = values[:, :width].astype(bf16).astype(f32)
        right = values[:, width : 2 * width].astype(bf16).astype(f32)
        return (left * jax.nn.sigmoid(right)).astype(bf16)

    @pl.when(pl.program_id(0) == 0)
    def _():
        place_pieces(offs, refs, weight, places, 0)
        rim[...] = gate(dot(before[...], weight[:, : 2 * width]))

    gated[...] = gate(dot(normed[...], weight[:, : 2 * width]))
    gate_out[...] = dot(normed[...], weight[:, 2 * width :]).astype(bf16)


def conv_project(normed, before, pieces, places, offs, width, gate_width):
    rows, depth = normed.shape
    total = 2 * width + gate_width
    tile = min(ROW_TILE, rows)
    return pl.pallas_call(
        functools.partial(conv_project_body, places=places),
        grid=(rows // tile,),
        in_specs=[SMEM, pl.BlockSpec((tile, depth), lambda i: (i, 0)), whole(before.shape)]
        + [whole(p.shape) for p in pieces],
        out_specs=[
            pl.BlockSpec((tile, width), lambda i: (i, 0)),
            pl.BlockSpec((tile, gate_width), lambda i: (i, 0)),
            whole((before.shape[0], width)),
        ],
        out_shape=[
            jax.ShapeDtypeStruct((rows, width), bf16),
            jax.ShapeDtypeStruct((rows, gate_width), bf16),
            jax.ShapeDtypeStruct((before.shape[0], width), bf16),
        ],
        scratch_shapes=[pltpu.VMEM((depth, total), bf16)],
        compiler_params=params(58),
        cost_estimate=pl.CostEstimate(
            flops=2 * rows * depth * total, bytes_accessed=rows * depth * 2, transcendentals=0
        ),
        name="conv_project",
    )(offs, normed, before, *pieces)


def conv_body(gated, rim, taps, out, sums, extended):
    rows, width = gated.shape
    count = taps.shape[0]
    first = HALO - count + 1
    chunk = 64
    extended[:HALO] = rim[...].astype(f32)
    extended[HALO : HALO + rows] = gated[...].astype(f32)
    extended[HALO + rows :] = jnp.zeros((8, width), f32)

    def step(i, carry):
        base = pl.multiple_of(i * chunk, chunk)
        there = pl.ds(base, chunk)
        total = jnp.zeros((chunk, LANES), f32)
        square = jnp.zeros((chunk, LANES), f32)
        for lane in range(0, width, LANES):
            here = slice(lane, lane + LANES)
            near = extended[pl.ds(base, chunk + HALO + 8), here]
            result = None
            for residue in range(8):
                acc = None
                for start in range(0, HALO + 1, 8):
                    tap = start + residue - first
                    if 0 <= tap < count:
                        part = taps[tap : tap + 1, here] * near[start : start + chunk + 8]
                        acc = part if acc is None else acc + part
                if residue:
                    acc = pltpu.roll(acc, chunk + 8 - residue, 0)
                acc = acc[:chunk]
                result = acc if result is None else result + acc
            out[there, here] = result.astype(bf16)
            total = total + result
            square = square + result * result
        sums[there, 0:1] = jnp.sum(total, axis=1, keepdims=True)
        sums[there, 1:2] = jnp.sum(square, axis=1, keepdims=True)
        return carry

    lax.fori_loop(0, rows // chunk, step, 0)


def convolve(gated, rim, taps):
    rows, width = gated.shape
    return pl.pallas_call(
        conv_body,
        out_shape=[
            jax.ShapeDtypeStruct((rows, width), bf16),
            jax.ShapeDtypeStruct((rows, 2), f32),
        ],
        scratch_shapes=[
            pltpu.VMEM((HALO + rows + 8, width), f32),
        ],
        compiler_params=pltpu.CompilerParams(vmem_limit_bytes=58 * 1024 * 1024),
        cost_estimate=pl.CostEstimate(
            flops=20 * rows * width * taps.shape[0], bytes_accessed=rows * width * 6, transcendentals=0
        ),
        name="convolve",
    )(gated, rim, taps)


def gla_body(query, keys, values, pre, bias, extra, local, since, held, packed, state, prefix):
    rows, channels = query.shape
    step = pl.program_id(0)
    group = min(2, channels // HK)
    kw, vw = HK * group, HV * group

    @pl.when(step == 0)
    def _():
        state[...] = jnp.zeros(state.shape, f32)
        prefix[...] = jnp.zeros(prefix.shape, f32)

    biased = pre[...] + bias[...]
    log_decay = (jnp.minimum(biased, 0.0) - jnp.log1p(jnp.exp(-jnp.abs(biased)))) / gate_divisor
    log_decay = log_decay + extra[...]
    at = lax.broadcasted_iota(jnp.int32, (rows, rows), 0)
    by = lax.broadcasted_iota(jnp.int32, (rows, rows), 1)
    causal = at >= by
    cum = jnp.dot(
        causal.astype(f32), log_decay, preferred_element_type=f32, precision=lax.Precision.HIGHEST
    )
    middle = cum[rows // 2 - 1 : rows // 2]
    end = cum[rows - 1 : rows]
    before = prefix[0:1]
    q = query[...].astype(f32) * HK ** (-0.5)
    k = keys[...].astype(f32)
    grown = jnp.exp(cum)
    q_mid = q * jnp.exp(cum - middle)
    k_mid = (k * jnp.exp(middle - cum)).astype(bf16)
    k_end = (k * jnp.exp(end - cum)).astype(bf16)
    q_run = q * grown
    since[...] = (q_run * jnp.exp(before)).astype(bf16)
    q_run = q_run.astype(bf16)
    end_decay = jnp.exp(end)
    key_row = lax.broadcasted_iota(jnp.int32, (kw, kw), 0)
    key_col = lax.broadcasted_iota(jnp.int32, (kw, kw), 1)
    lane = lax.broadcasted_iota(jnp.int32, (rows, kw), 1)
    own_head = (
        lax.broadcasted_iota(jnp.int32, (kw, vw), 0) // HK
        == lax.broadcasted_iota(jnp.int32, (kw, vw), 1) // HV
    )
    for p in range(channels // kw):
        ks = slice(p * kw, (p + 1) * kw)
        v = values[:, p * vw : (p + 1) * vw]
        s = state[p]
        carried = dot(q_run[:, ks], s.astype(bf16))
        for h in range(group):
            q_head = jnp.where(lane // HK == h, q_mid[:, ks], 0.0).astype(bf16)
            scores = lax.dot_general(
                q_head, k_mid[:, ks], (((1,), (1,)), ((), ())), preferred_element_type=f32
            )
            scores = jnp.where(causal, scores, 0.0).astype(bf16)
            hs = slice(h * HV, (h + 1) * HV)
            first = p * vw + h * HV
            local[:, first : first + HV] = (dot(scores, v[:, hs]) + carried[:, hs]).astype(bf16)
        column = jnp.sum(jnp.where(key_row == key_col, end_decay[:, ks], 0.0), axis=1, keepdims=True)
        added = lax.dot_general(
            k_end[:, ks], v, (((0,), (0,)), ((), ())), preferred_element_type=f32
        )
        state[p] = s * column + jnp.where(own_head, added, 0.0)
    prefix[0:1] = before + end

    @pl.when(step == pl.num_programs(0) - 1)
    def _():
        everything = prefix[0:1]
        for p in range(channels // kw):
            column = jnp.sum(
                jnp.where(key_row == key_col, everything[:, p * kw : (p + 1) * kw], 0.0), axis=1, keepdims=True
            )
            held[p * kw : (p + 1) * kw, 3 * HV :] = jnp.broadcast_to(column, (kw, HV))
            for h in range(group):
                row = p * kw + h * HK
                own = state[p, h * HK : (h + 1) * HK, h * HV : (h + 1) * HV]
                held[row : row + HK, 2 * HV : 3 * HV] = own
        held[:, : 2 * HV] = jnp.zeros((channels, 2 * HV), f32)
        packed[:, :HV], packed[:, HV:] = packing(held[:, 2 * HV : 3 * HV], held[:, 3 * HV :])


def linear_attention(query, keys, values, pre, bias, extra):
    rows, channels = query.shape
    wide = values.shape[1]
    group = min(2, channels // HK)
    tile = min(BLOCK, rows)
    narrow = pl.BlockSpec((tile, channels), lambda i: (i, 0))
    broad = pl.BlockSpec((tile, wide), lambda i: (i, 0))
    return pl.pallas_call(
        gla_body,
        grid=(rows // tile,),
        in_specs=[narrow, narrow, broad, narrow, whole((1, channels)), narrow],
        out_specs=[broad, narrow, whole((channels, 4 * HV)), whole((channels, 2 * HV))],
        out_shape=[
            jax.ShapeDtypeStruct((rows, wide), bf16),
            jax.ShapeDtypeStruct((rows, channels), bf16),
            jax.ShapeDtypeStruct((channels, 4 * HV), f32),
            jax.ShapeDtypeStruct((channels, 2 * HV), bf16),
        ],
        scratch_shapes=[
            pltpu.VMEM((channels // HK // group, HK * group, HV * group), f32),
            pltpu.VMEM((8, channels), f32),
        ],
        compiler_params=params(24),
        cost_estimate=pl.CostEstimate(
            flops=20 * rows * tile * wide, bytes_accessed=rows * wide * 8, transcendentals=0
        ),
        name="linear_attention",
    )(query, keys, values, pre, bias, extra)


def packing(state, logs):
    high = logs.astype(bf16)
    lane = lax.broadcasted_iota(jnp.int32, logs.shape, 1)
    low = (logs - high.astype(f32)).astype(bf16)
    return state.astype(bf16), jnp.where(lane < HV // 2, high.astype(f32), low.astype(f32)).astype(bf16)


def unpacking(packed):
    half = packed[:, HV : 2 * HV].astype(f32)
    logs = half[:, 0:1] + half[:, HV // 2 : HV // 2 + 1]
    return packed[:, :HV].astype(f32), jnp.broadcast_to(logs, half.shape)


def combine_body(upper, packed, held, held_out, packed_out):
    state, logs = unpacking(packed)
    above = upper[0] == 1
    pre, pre_logs, own, own_logs = (held[:, k * HV : (k + 1) * HV] for k in range(4))
    held_out[:, :HV] = jnp.where(above, jnp.exp(pre_logs) * state + pre, pre)
    held_out[:, HV : 2 * HV] = jnp.where(above, pre_logs + logs, pre_logs)
    joined = jnp.where(above, jnp.exp(own_logs) * state + own, jnp.exp(logs) * own + state)
    joined_logs = own_logs + logs
    held_out[:, 2 * HV : 3 * HV] = joined
    held_out[:, 3 * HV :] = joined_logs
    packed_out[:, :HV], packed_out[:, HV:] = packing(joined, joined_logs)


def combine(upper, packed, held):
    vmem = pl.BlockSpec(memory_space=pltpu.VMEM)
    return pl.pallas_call(
        combine_body,
        in_specs=[SMEM, vmem, vmem],
        out_specs=[vmem, vmem],
        out_shape=[
            jax.ShapeDtypeStruct(held.shape, f32),
            jax.ShapeDtypeStruct(packed.shape, bf16),
        ],
        compiler_params=pltpu.CompilerParams(vmem_limit_bytes=4 * 1024 * 1024),
        name="combine",
    )(upper, packed, held)


def enter_body(upper, packed, held, init, out):
    last, logs = unpacking(packed)
    above = upper[0] == 1
    pre, pre_logs = held[:, :HV], held[:, HV : 2 * HV]
    started = jnp.where(above, jnp.exp(pre_logs) * last + pre, pre)
    logs = jnp.where(above, pre_logs + logs, pre_logs)
    out[...] = (started + jnp.exp(logs) * init[...]).astype(bf16)


def enter(held, packed, upper, init):
    vmem = pl.BlockSpec(memory_space=pltpu.VMEM)
    return pl.pallas_call(
        enter_body,
        in_specs=[SMEM, vmem, vmem, vmem],
        out_specs=vmem,
        out_shape=jax.ShapeDtypeStruct(init.shape, bf16),
        compiler_params=pltpu.CompilerParams(vmem_limit_bytes=4 * 1024 * 1024),
        name="enter",
    )(upper, packed, held, init)


def finish_body(start, offs, *refs, channels, parts, places):
    sums, refs = refs[:parts], refs[parts:]
    conv, conv_gain, local, since, state, gate, head_gain, *refs = refs
    weights, (out, act) = refs[: len(places)], refs[len(places) :]
    width = conv.shape[1]
    stats = sums[0][...]
    for more in sums[1:]:
        stats = stats + more[...]
    mean_val = stats[:, 0:1] / channels
    square_mean = stats[:, 1:2] / channels
    normal = (conv[...].astype(f32) - mean_val) * lax.rsqrt(square_mean - mean_val * mean_val + epsilon)
    normal = normal * conv_gain[...]
    act[:, :width] = (normal * jax.nn.sigmoid(normal)).astype(bf16)
    keys = since.shape[1]
    group = min(2, keys // HK)
    kw = HK * group
    lane = lax.broadcasted_iota(jnp.int32, (since.shape[0], kw), 1)
    for head in range(keys // HK):
        p, h = divmod(head, group)
        q = jnp.where(lane // HK == h, since[:, p * kw : (p + 1) * kw].astype(f32), 0.0).astype(bf16)
        hs = slice(head * HV, (head + 1) * HV)
        attn = local[:, hs].astype(f32) + dot(q, state[p * kw : (p + 1) * kw])
        attn = attn * lax.rsqrt(jnp.mean(attn * attn, axis=1, keepdims=True) + epsilon)
        gated = gate[:, hs].astype(f32)
        gated = gated * jax.nn.sigmoid(gated)
        act[:, width + head * HV : width + (head + 1) * HV] = (attn * head_gain[...] * gated).astype(bf16)
    for ref, spots in zip(weights, places):
        size = ref.shape[1] // len(spots)
        values = dot(act[...], ref[...]).astype(bf16)
        for k, spot in enumerate(spots):
            there = pl.ds(pl.multiple_of(offs[spot], size), size)
            out[:, there] = values[:, k * size : (k + 1) * size]


def finish(first, rows, sums, conv, conv_gain, local, since, state, gate, head_gain, out_weights, total, channels):
    pieces, places, offs = out_weights
    width, wide = conv.shape[1], local.shape[1]
    tile = min(ROW_TILE, rows)
    start = (first // tile).astype(jnp.int32).reshape(1)

    def tiled(cols):
        return pl.BlockSpec((tile, cols), lambda i, at: (at[0] + i, 0))

    def fixed(shape):
        return pl.BlockSpec(shape, lambda i, at: (0, 0))

    spec = pltpu.PrefetchScalarGridSpec(
        num_scalar_prefetch=1,
        grid=(rows // tile,),
        in_specs=[SMEM]
        + [tiled(2) for _ in sums]
        + [
            tiled(width),
            fixed((1, width)),
            tiled(wide),
            tiled(since.shape[1]),
            fixed(state.shape),
            tiled(wide),
            fixed((1, HV)),
        ]
        + [pl.BlockSpec(memory_space=pltpu.VMEM) for _ in pieces],
        out_specs=pl.BlockSpec((tile, total), lambda i, at: (i, 0)),
        scratch_shapes=[pltpu.VMEM((tile, width + wide), bf16)],
    )
    return pl.pallas_call(
        functools.partial(finish_body, channels=channels, parts=len(sums), places=places),
        grid_spec=spec,
        out_shape=jax.ShapeDtypeStruct((rows, total), bf16),
        compiler_params=params(56),
        cost_estimate=pl.CostEstimate(
            flops=2 * rows * (width + wide) * total, bytes_accessed=rows * total * 2, transcendentals=0
        ),
        name="finish",
    )(start, offs, *sums, conv, conv_gain, local, since, state, gate, head_gain, *pieces)


def normed_rows(own, axis, norm_gain):
    if lax.axis_size(axis) != 2:
        full = lax.all_gather(own, axis, axis=1, tiled=True)
        return normalize([full], jnp.zeros((1,), jnp.int32), norm_gain)
    other = flip(own, axis, 1)
    mine = lax.axis_index(axis)
    places = jnp.stack([mine, 1 - mine]).astype(jnp.int32) * own.shape[1]
    return normalize([own, other], places, norm_gain)


def per_device(
    tokens,
    norm_gain,
    w_conv_a,
    w_conv_gate,
    conv_weight,
    conv_gain,
    w_query,
    w_key,
    w_value,
    w_outgate,
    w_decay,
    decay_bias,
    decay_extra,
    head_gain,
    init_state,
    w_out_conv,
    w_out_gla,
):
    rows = tokens.shape[0]
    groups = lax.axis_size("tp")
    width = w_conv_a.shape[1]
    channels = w_query.shape[1]
    wide = w_value.shape[1]

    gla_own = jnp.concatenate([w_query, w_key, w_value, w_decay], axis=1)
    conv_own = jnp.concatenate([w_conv_a, w_conv_gate, w_outgate], axis=1)
    out_own = jnp.concatenate([w_out_conv, w_out_gla], axis=0)
    gla_weights = gathered(gla_own, "sp", 0, 0, "single")
    conv_weights = gathered(conv_own, "sp", 0, 0, "double")
    out_weights = gathered(out_own, "sp", 1, 1, "double")

    rim = shifted(tokens[rows - HALO :], "sp", 1)
    normed = normed_rows(tokens, "tp", norm_gain)
    normed_rim = normed_rows(rim, "tp", norm_gain)

    query, keys, values, decay_pre = project(
        normed, *gla_weights, (channels, channels, wide, channels), (bf16, bf16, bf16, f32)
    )
    local, since, *end = linear_attention(
        query, keys, values, decay_pre, decay_bias[None, :], decay_extra
    )
    before = entering(*end, "sp")

    gated, gate, gated_rim = conv_project(normed, normed_rim, *conv_weights, width, wide)
    conv, sums = convolve(gated, gated_rim, conv_weight)
    sums = [sums, flip(sums, "tp", 1)] if groups == 2 else [lax.psum(sums, "tp")]

    state = enter(*before, init_state.reshape(channels, HV))
    total = norm_gain.shape[0]

    def rows_from(first, count):
        return finish(
            jnp.asarray(first),
            count,
            sums,
            conv,
            conv_gain[None, :],
            local,
            since,
            state,
            gate,
            head_gain[None, :],
            out_weights,
            total,
            width * groups,
        )

    if groups != 2:
        return lax.psum_scatter(rows_from(0, rows), "tp", scatter_dimension=0, tiled=True)
    half = rows // 2
    mine = lax.axis_index("tp")
    received = flip(rows_from((1 - mine) * half, half), "tp", 1)
    kept = rows_from(mine * half, half)
    return (kept.astype(f32) + received.astype(f32)).astype(bf16)


def solution(mesh):
    placed = (
        P("sp", "tp"),
        P(),
        P("sp", "tp"),
        P("sp", "tp"),
        P(None, "tp"),
        P("tp"),
        P("sp", "tp"),
        P("sp", "tp"),
        P("sp", "tp"),
        P("sp", "tp"),
        P("sp", "tp"),
        P("tp"),
        P("sp", "tp"),
        P(),
        P("tp", None, None),
        P("tp", "sp"),
        P("tp", "sp"),
    )

    return jax.shard_map(
        per_device, mesh=mesh, in_specs=placed, out_specs=P(("sp", "tp"), None), check_vma=False
    )
```
